32 devices in a mesh: kv: 8 (over z, y), tp: 4 (over x, core).
Axes of the slice: x: 2, y: 2, z: 4, core: 2. Of those that a mesh axis runs over, the one named last changes fastest.
Arguments:
- tokens: bfloat16 [4096, 2048], P('kv', 'tp'), may hold values from -9 to 9
- w_query: bfloat16 [2048, 1536], P(None, 'tp'), may hold values from -1 to 1
- w_key: bfloat16 [2048, 1536], P(None, 'tp'), may hold values from -1 to 1
- w_value: bfloat16 [2048, 1536], P(None, 'tp'), may hold values from -0.5 to 0.5
- w_out: bfloat16 [1536, 2048], P('tp'), may hold values from -0.15625 to 0.15625
- chosen: int32 [128, 24], P('kv'), may hold values from 0 to 127, as said below
Outputs:
- mixed: bfloat16 [4096, 2048], P(('kv', 'tp'))
The draws below stay inside these ranges and needn't reach their ends.
Inputs may be any that keep to these rules, and one draw needn't show every extreme that they name: `chosen`: row c names blocks no later than c; its first entry is c and its second c - 1 (0 for row 0), and an entry may repeat. Taking the rows in aligned runs of 16, one run for each index of kv, the rows of one run name at most 2 distinct blocks lying in any one other index's positions; in every draw some index of kv names exactly 2 from every earlier index. Every run names some block of the index just before it and of the index half the axis before it, where those exist.
All inputs are finite; a program needn't handle non-finite values.
Results may differ from the reference program's by a relative error of at most 0.014.
Values may be sent and summed in bfloat16 or wider, within the bound.
A program may use at most 320 MiB of HBM per device.

```python
import math
import jax
import jax.numpy as jnp
from jax import lax

D = 2048
HEADS = 12
HD = 128
BLK = 32
SEL = 24
MOST = 2
TOK_DEV = 512
TOKENS = 4096
N_KV = 8
N_TP = 4


def draw_tokens(key, part):
    base_key = jax.random.fold_in(key, 7)
    first, second, third = jax.random.split(base_key, 3)
    values = jnp.clip(jax.random.normal(first, (TOKENS, D), jnp.float32), -8.0, 8.0)
    return values.astype(jnp.bfloat16)


def weight_pair(key):
    first = jax.random.normal(jax.random.fold_in(key, 101), (D, HEADS * HD), jnp.float32) / math.sqrt(D)
    second = jax.random.normal(jax.random.fold_in(key, 102), (D, HEADS * HD), jnp.float32) / math.sqrt(D)
    return (first, second)


def draw_w_query(key, part):
    first, second = weight_pair(key)
    return jnp.clip(2.0 * first, -1.0, 1.0).astype(jnp.bfloat16)


def draw_w_key(key, part):
    first, second = weight_pair(key)
    values = second
    return jnp.clip(values, -1.0, 1.0).astype(jnp.bfloat16)


def draw_chosen(key, part):
    per_dev = TOK_DEV // BLK
    ndevs = N_KV
    nblocks = per_dev * ndevs
    keys = jax.random.split(jax.random.fold_in(key, 11), 7)
    popular = jnp.maximum(jax.random.randint(keys[0], (nblocks,), 0, 8) - 4, 0)
    noise = jax.random.randint(keys[1], (nblocks,), 0, 4096)
    block_ids = jnp.arange(nblocks, dtype=jnp.int32)
    score = popular * (1 << 24) + noise * 256 + block_ids % per_dev
    devices = jnp.arange(ndevs, dtype=jnp.int32)
    full_dev = jax.random.randint(keys[2], (), 1, ndevs)
    extra_full = jax.random.randint(keys[3], (ndevs,), 0, 4) == 0
    counts = jax.random.randint(keys[4], (ndevs, ndevs), 0, MOST + 1)
    is_full = (devices == full_dev) | extra_full
    counts = jnp.where(is_full[:, None], MOST, counts)
    before = devices[None, :] == devices[:, None] - 1
    halfway = devices[None, :] == devices[:, None] - ndevs // 2
    counts = jnp.where(before | halfway, jnp.maximum(counts, 1), counts)
    counts = jnp.where(devices[None, :] < devices[:, None], counts, 0)
    boost = (block_ids[None, :] == devices[:, None] * per_dev - 1).astype(jnp.int32) * (1 << 30)
    dev_score = (score[None, :] + boost).reshape(ndevs, ndevs, per_dev)
    ranks = jnp.sum((dev_score[:, :, None, :] > dev_score[:, :, :, None]).astype(jnp.int32), axis=-1)
    in_pool = (ranks < counts[:, :, None]).reshape(ndevs, nblocks)
    pool_pos = jnp.cumsum(in_pool.astype(jnp.int32), axis=1) - 1
    pool_size = jnp.sum(in_pool.astype(jnp.int32), axis=1)
    fill_slots = SEL - 2
    places = jnp.arange(fill_slots * per_dev, dtype=jnp.int32)
    hit = in_pool[:, None, :] & (pool_pos[:, None, :] == places[None, :, None])
    elements = jnp.sum(hit.astype(jnp.int32) * block_ids[None, None, :], axis=-1)
    rows_in = jnp.arange(per_dev, dtype=jnp.int32)
    slot_in = jnp.arange(fill_slots, dtype=jnp.int32)
    place_idx = slot_in[None, :] * per_dev + rows_in[:, None]
    random_pick = jax.random.randint(keys[5], (ndevs, per_dev, fill_slots), 0, 1 << 20)
    safe_size = jnp.maximum(pool_size, 1)[:, None, None]
    take = jnp.where(place_idx[None] < pool_size[:, None, None], place_idx[None], random_pick % safe_size)
    picked = jnp.take_along_axis(elements, take.reshape(ndevs, -1), axis=1).reshape(ndevs, per_dev, fill_slots)
    own_block = devices[:, None] * per_dev + rows_in[None, :]
    own_fill = devices[:, None, None] * per_dev + random_pick % (rows_in[None, :, None] + 1)
    filled = jnp.where(pool_size[:, None, None] > 0, picked, own_fill)
    prev_block = jnp.maximum(own_block - 1, 0)
    rows = jnp.concatenate([own_block[:, :, None], prev_block[:, :, None], filled], axis=-1)
    return rows.reshape(nblocks, SEL).astype(jnp.int32)


def steps_of(rng, dims, cuts, low, top_value):
    def one(axis_at, parts):
        steps = jax.random.uniform(jax.random.fold_in(jax.random.fold_in(rng, 6), axis_at), (parts,), jnp.float32, low / len(cuts), top_value / len(cuts))
        return jnp.repeat(jnp.exp(steps), dims[axis_at] // parts).reshape((-1,) + (1,) * (len(dims) - axis_at - 1))

    gain = one(*cuts[0])
    for cut in cuts[1:]:
        gain = gain * one(*cut)
    return gain


def gaussian(rng, extent, width, limit, cuts=(), kind=jnp.bfloat16):
    gain = steps_of(rng, extent, cuts, -0.22, 0.18) if cuts else 1.0
    values = jax.random.normal(rng, extent, jnp.float32) * width * gain
    return jnp.minimum(jnp.maximum(values, -limit), limit).astype(kind)


def setup_inputs(seed: int = 0) -> dict:
    key_of = jax.random.split(jax.random.key(seed), 7)
    tokens = draw_tokens(jax.random.fold_in(key_of[6], 71), 0)
    w_query = draw_w_query(jax.random.fold_in(key_of[6], 71), 0)
    w_key = draw_w_key(jax.random.fold_in(key_of[6], 71), 0)
    w_value = gaussian(key_of[3], (D, HEADS * HD), (D // 16) ** -0.5, 0.5, ((1, 4),))
    w_out = gaussian(key_of[4], (HEADS * HD, D), (HEADS * HD) ** -0.5, 0.15625, ((0, 4),))
    chosen = draw_chosen(jax.random.fold_in(key_of[6], 71), 0)
    return {"tokens": tokens, "w_query": w_query, "w_key": w_key, "w_value": w_value, "w_out": w_out, "chosen": chosen}


NEG = -1e30


def reference(tokens, w_query, w_key, w_value, w_out, chosen):
    query_rows = jnp.dot(tokens, w_query, preferred_element_type=jnp.float32).astype(jnp.bfloat16)
    key_rows = jnp.dot(tokens, w_key, preferred_element_type=jnp.float32).astype(jnp.bfloat16)
    value_rows = jnp.dot(tokens, w_value, preferred_element_type=jnp.float32).astype(jnp.bfloat16)
    total_rows = tokens.shape[0]
    block_count = total_rows // BLK
    query_blocks = query_rows.reshape(block_count, BLK, HEADS, HD)
    key_blocks = key_rows.reshape(block_count, BLK, HEADS, HD)
    value_blocks = value_rows.reshape(block_count, BLK, HEADS, HD)
    offsets = jnp.arange(BLK, dtype=jnp.int32)
    slot_ids = jnp.arange(SEL, dtype=jnp.int32)
    earlier_slot = slot_ids[None, :] < slot_ids[:, None]

    def one_block(packed):
        query_block, chosen_row, block_index = packed
        repeat_slot = jnp.any((chosen_row[:, None] == chosen_row[None, :]) & earlier_slot, axis=1)
        gathered_keys = key_blocks[chosen_row].astype(jnp.float32)
        gathered_values = value_blocks[chosen_row].astype(jnp.float32)
        scores = jnp.einsum('qhd,jkhd->hqjk', query_block.astype(jnp.float32), gathered_keys) * (HD ** -0.5)
        key_pos = chosen_row[:, None] * BLK + offsets[None, :]
        query_pos = block_index * BLK + offsets
        allowed = (~repeat_slot)[None, :, None] & (key_pos[None, :, :] <= query_pos[:, None, None])
        scores = jnp.where(allowed[None], scores, NEG)
        weights = jax.nn.softmax(scores.reshape(HEADS, BLK, SEL * BLK), axis=-1).reshape(HEADS, BLK, SEL, BLK)
        mixed_heads = jnp.einsum('hqjk,jkhd->qhd', weights, gathered_values)
        return mixed_heads.astype(jnp.bfloat16).reshape(BLK, HEADS * HD)

    attended = lax.map(one_block, (query_blocks, chosen, jnp.arange(block_count, dtype=jnp.int32)))
    attended = attended.reshape(total_rows, HEADS * HD)
    group_width = HEADS * HD // N_TP
    summed = jnp.zeros((total_rows, w_out.shape[1]), jnp.float32)
    for group in range(N_TP):
        partial_value = jnp.dot(attended[:, group * group_width:(group + 1) * group_width],
                          w_out[group * group_width:(group + 1) * group_width],
                          preferred_element_type=jnp.float32).astype(jnp.bfloat16)
        partial_value = lax.optimization_barrier(partial_value)
        summed = summed + partial_value.astype(jnp.float32)
    return summed.astype(jnp.bfloat16)
```

```python
import functools

import jax
import jax.numpy as jnp
from jax import lax
from jax.experimental import pallas as pl
from jax.experimental.pallas import tpu as pltpu
from jax.sharding import PartitionSpec as P

HD = 128
BLK = 32
MOST = 2
NEG = -1e30
LOG2E = 1.4426950408889634
BF = jnp.bfloat16
F32 = jnp.float32
MESH = pl.DeviceIdType.MESH
CHUNKS = 4
OUT_CHUNKS = 4
VMEM_MIB = 60
scope = jax.named_scope


def dot(a, b):
    return jnp.dot(a, b, preferred_element_type=F32)


def dot_nt(a, b):
    return lax.dot_general(a, b, (((1,), (1,)), ((), ())), preferred_element_type=F32)


def quot(x, size):
    if size & (size - 1) == 0:
        return lax.shift_right_logical(x, jnp.full(x.shape, size.bit_length() - 1, x.dtype))
    return lax.div(x, size)


def rest(x, size):
    if size & (size - 1) == 0:
        return x & (size - 1)
    return lax.rem(x, size)


def iota(shape, dim):
    return lax.broadcasted_iota(jnp.int32, shape, dim)


def ones_where(cond):
    return cond.astype(F32).astype(BF)


def kernel(
    n, tok, wq, wk, wv, wo, chosen, out,
    rowsel, wbuf, wobuf, gat, far, pick, pickf, ask, asked, choice, qkv, kvf,
    bias, biasf, top, tot, summed, att, psend, precv, part_x, xsend, xrecv, mine,
    wsem, ox_s, ox_r, oc_s, oc_r, of_s, of_r, rq_s, rq_r, fk_s, fk_r,
    fx_s, fx_r, fc_s, fc_r, ff_s, ff_r, pd_s, pd_r, px_s, px_r,
):
    rows, feat = tok.shape
    width = wq.shape[1]
    heads = width // HD
    per = rows // BLK
    blocks = n * per
    slot = MOST * BLK
    spots = kvf.shape[0]
    cols = wo.shape[1]
    quarter = rows // 4
    piece = rows // CHUNKS
    me = lax.axis_index("kv")
    t = lax.axis_index("tp")
    mate = t + 1 - 2 * lax.rem(t, 2)
    across = lax.rem(t + 2, 4)
    diag = lax.rem(mate + 2, 4)
    last = n - 1
    near = n // 2
    reach = last - near

    def lanes(d):
        return pl.ds(pl.multiple_of(d * feat, feat), feat)

    def remote(src, dst, s, r, who):
        return pltpu.make_async_remote_copy(
            src_ref=src, dst_ref=dst, send_sem=s, recv_sem=r, device_id=who, device_id_type=MESH
        )

    barrier = pltpu.get_barrier_semaphore()
    for d in (mate, across, diag):
        pl.semaphore_signal(barrier, inc=1, device_id=(me, d), device_id_type=MESH)
    for k in range(1, n):
        pl.semaphore_signal(
            barrier, inc=1, device_id=(lax.rem(me + k, n), t), device_id_type=MESH
        )

    list_load = pltpu.make_async_copy(chosen, rowsel, wsem.at[5])
    list_load.start()
    tok_load = pltpu.make_async_copy(tok, gat.at[:, lanes(t)], wsem.at[0])
    tok_load.start()
    loads = []
    for j, w in enumerate((wq, wk, wv)):
        c = pltpu.make_async_copy(w, wbuf.at[:, pl.ds(j * width, width)], wsem.at[1 + j])
        c.start()
        loads.append(c)
    wo_load = pltpu.make_async_copy(wo, wobuf, wsem.at[4])
    wo_load.start()

    with scope("ask"):
        lane = iota((per, blocks), 1)
        seen = jnp.zeros((per, blocks), jnp.int32)
        list_load.wait()
        picks = rowsel[...]
        for j in range(picks.shape[1]):
            seen = jnp.maximum(seen, (picks[:, j : j + 1] == lane).astype(jnp.int32))
        wanted = jnp.max(seen, axis=0, keepdims=True)
        lane1 = iota((1, blocks), 1)
        inside = (lane1 >= me * per) & (lane1 < me * per + per)
        wanted = jnp.where(inside, 0, wanted).astype(F32)
        ia, ib = iota((blocks, blocks), 0), iota((blocks, blocks), 1)
        tri = ones_where((quot(ia, per) == quot(ib, per)) & (ia <= ib))
        rank = dot(jnp.broadcast_to(wanted, (8, blocks)).astype(BF), tri)[0:1, :] * wanted
        pad = max(n, 8)
        owner = quot(iota((pad, blocks), 1), per) == iota((pad, blocks), 0)
        ranks = jnp.where(owner, jnp.broadcast_to(rank, (pad, blocks)), 0.0).astype(BF)
        within = ones_where(
            rest(iota((blocks, rows), 0), per) == quot(iota((blocks, rows), 1), BLK)
        )
        places = dot(ranks, within)
        for s in range(n):
            ask[s] = jnp.broadcast_to(places[s : s + 1, :], (8, rows))

    tok_load.wait()
    with scope("barrier"):
        pl.semaphore_wait(barrier, n + 2)

    own_x, own_f = [], []
    for c in range(CHUNKS):
        part = pl.ds(c * piece, piece)
        src = gat.at[part, lanes(t)]
        own_x.append(remote(src, src, ox_s.at[c], ox_r.at[c], (me, across)))
        own_x[-1].start()
    whole = gat.at[:, lanes(t)]
    own_c = remote(whole, whole, oc_s, oc_r, (me, mate))
    own_c.start()

    asks = []
    for k in range(1, n):
        low = lax.max(me - k, 0)
        c = remote(ask.at[low], asked.at[k - 1], rq_s.at[k - 1], rq_r.at[k - 1], (low, t))
        pl.when(me >= k)(c.start)
        asks.append(c)

    with scope("bias"):
        seen_b = seen.astype(F32).astype(BF)
        spread = ones_where(iota((blocks, rows), 0) == me * per + quot(iota((blocks, rows), 1), BLK))
        col = iota((spots, blocks), 0)
        blk = iota((spots, blocks), 1)
        hit = ones_where(
            (quot(col, slot) == quot(blk, per))
            & (
                jnp.broadcast_to(rank, (spots, blocks))
                == (quot(rest(col, slot), BLK) + 1).astype(F32)
            )
        )
        far_seen = dot_nt(seen_b, hit)
        grow = ones_where(quot(iota((rows, per), 0), BLK) == iota((rows, per), 1))
        own_seen = dot(grow, dot(seen_b, spread).astype(BF))
        causal = iota((rows, rows), 1) <= iota((rows, rows), 0)
        bias[...] = jnp.where((own_seen > 0.5) & causal, 0.0, NEG)
        biasf[...] = jnp.where(dot(grow, far_seen.astype(BF)) > 0.5, 0.0, NEG)
        for s in range(last):
            part = pl.ds(s * slot, slot)
            if s < near:

                @pl.when(me <= s)
                def _():
                    far[part, :] = jnp.zeros((slot, far.shape[1]), BF)

            @pl.when(me <= s)
            def _():
                kvf[part, :] = jnp.zeros((slot, kvf.shape[1]), BF)

    with scope("picks"):
        srow, scol = iota((slot, rows), 0), iota((slot, rows), 1)
        same = rest(srow, BLK) == rest(scol, BLK)
        want_rank = (quot(srow, BLK) + 1).astype(F32)
        sends = {}

        def select(k):
            sel = same & (asked[k - 1, 0:1, :] == want_rank)
            return ones_where(sel)

        def token_send(k):
            sends[k] = remote(
                pick.at[k - 1],
                far.at[pl.ds(pl.multiple_of(lax.min(me, near - 1) * slot, slot), slot), lanes(t)],
                fk_s.at[k - 1],
                fk_r.at[me],
                (lax.rem(me + k, n), t),
            )

            @pl.when((me < near) & (me + k < n))
            def _():
                asks[k - 1].wait_recv()
                pick[k - 1] = dot(select(k), gat[:, lanes(t)]).astype(BF)
                sends[k].start()

        for k in range(last, 0, -1):
            token_send(k)

        @pl.when(me >= near)
        def _():
            for k in range(1, reach + 1):

                @pl.when(me + k < n)
                def _():
                    asks[k - 1].wait_recv()
                    choice[pl.ds((k - 1) * slot, slot), :] = select(k)

                @pl.when(me + k >= n)
                def _():
                    choice[pl.ds((k - 1) * slot, slot), :] = jnp.zeros((slot, rows), BF)

    scale = HD ** (-0.5) * LOG2E
    cut = [slice(h * HD, (h + 1) * HD) for h in range(heads)]

    def head(j, h):
        return slice(j * width + h * HD, j * width + (h + 1) * HD)

    def project(c):
        rr = slice(c * piece, (c + 1) * piece)
        val = dot(gat[rr, :], wbuf[...])
        qkv[rr, :width] = (val[:, :width] * scale).astype(BF)
        qkv[rr, width:] = val[:, width:].astype(BF)

    def attend(c):
        rr = slice(c * piece, (c + 1) * piece)
        upto = (c + 1) * piece
        shade = bias[rr, :upto]
        ss = [dot_nt(qkv[rr, head(0, h)], qkv[:upto, head(1, h)]) + shade for h in range(heads)]
        ms = [jnp.max(x, axis=1, keepdims=True) for x in ss]
        ps = [jnp.exp2(x - m) for x, m in zip(ss, ms)]
        vals = [dot(p.astype(BF), qkv[:upto, head(2, h)]) for h, p in enumerate(ps)]
        for h in range(heads):
            top[h, rr, :] = ms[h]
            tot[h, rr, :] = jnp.sum(ps[h], axis=1, keepdims=True)
            summed[h, rr, :] = vals[h]

    near_sends = []

    def send_near():
        for k in range(1, reach + 1):
            part = pl.ds((k - 1) * slot, slot)
            near_sends.append(
                remote(
                    pickf.at[part],
                    kvf.at[pl.ds(pl.multiple_of(me * slot, slot), slot)],
                    fk_s.at[k - 1],
                    fk_r.at[me],
                    (lax.rem(me + k, n), t),
                )
            )

        @pl.when((me >= near) & (me < last))
        def _():
            pickf[...] = dot(choice[...], qkv[:, width:]).astype(BF)
            for k in range(1, reach + 1):
                pl.when(me + k < n)(near_sends[k - 1].start)

    def take_near():
        for s in range(near, last):

            @pl.when(me > s)
            def _():
                here = kvf.at[slot_of(s)]
                remote(here, here, fk_s.at[0], fk_r.at[s], (me, t)).wait_recv()

    far_x, far_c, far_f = [], [], []

    def slot_of(s):
        return pl.ds(s * slot, slot)

    def hand(s):
        here = far.at[slot_of(s), lanes(t)]
        far_x.append(remote(here, here, fx_s.at[s], fx_r.at[s], (me, across)))
        far_c.append(remote(here, here, fc_s.at[s], fc_r.at[s], (me, mate)))

        @pl.when(me > s)
        def _():
            remote(pick.at[0], here, fk_s.at[0], fk_r.at[s], (me, t)).wait_recv()
            far_x[s].start()
            far_c[s].start()

    def hand_on(s):
        theirs = far.at[slot_of(s), lanes(across)]
        far_f.append(remote(theirs, theirs, ff_s.at[s], ff_r.at[s], (me, mate)))

        @pl.when(me > s)
        def _():
            far_x[s].wait_recv()
            far_f[s].start()

    def project_far(lo, hi):
        @pl.when(me > lo)
        def _():
            for s in range(lo, hi):

                @pl.when(me > s)
                def _():
                    far_c[s].wait_recv()
                    far_f[s].wait_recv()

            part = slice(lo * slot, hi * slot)
            kvf[part, :] = dot(far[part, :], wbuf[:, width:]).astype(BF)

    def absorb(part, lo, hi):
        keys = slice(lo * slot, hi * slot)
        shade = biasf[part, keys]
        ss = [dot_nt(qkv[part, head(0, h)], kvf[keys, cut[h]]) + shade for h in range(heads)]
        old = [top[h, part, :] for h in range(heads)]
        ms = [jnp.maximum(m, jnp.max(x, axis=1, keepdims=True)) for m, x in zip(old, ss)]
        ps = [jnp.exp2(x - m) for x, m in zip(ss, ms)]
        keep = [jnp.exp2(m0 - m) for m0, m in zip(old, ms)]
        vals = [dot(p.astype(BF), kvf[keys, width + h * HD : width + (h + 1) * HD]) for h, p in enumerate(ps)]
        totals = [tot[h, part, :] * keep[h] + jnp.sum(ps[h], axis=1, keepdims=True) for h in range(heads)]
        sums = [summed[h, part, :] * keep[h] + vals[h] for h in range(heads)]
        return ms, totals, sums

    def absorb_early(lo, hi):
        @pl.when(me > lo)
        def _():
            for r in range(2):
                part = slice(2 * r * quarter, 2 * (r + 1) * quarter)
                ms, totals, sums = absorb(part, lo, hi)
                for h in range(heads):
                    top[h, part, :] = ms[h]
                    tot[h, part, :] = totals[h]
                    summed[h, part, :] = sums[h]

    def finish(lo, hi, *whos):
        parts = [pl.ds(pl.multiple_of(who * quarter, quarter), quarter) for who in whos]

        @pl.when(me > lo)
        def _():
            for part in parts:
                _, totals, sums = absorb(part, lo, hi)
                for h in range(heads):
                    att[part, cut[h]] = (sums[h] / totals[h]).astype(BF)

        @pl.when(me <= lo)
        def _():
            for part in parts:
                for h in range(heads):
                    att[part, cut[h]] = (summed[h, part, :] / tot[h, part, :]).astype(BF)

        return parts

    for c in loads:
        c.wait()

    with scope("own_c"):
        own_c.wait_recv()

    def take(c):
        own_x[c].wait_recv()
        theirs = gat.at[pl.ds(c * piece, piece), lanes(across)]
        own_f.append(remote(theirs, theirs, of_s.at[c], of_r.at[c], (me, mate)))
        own_f[c].start()

    for c in range(CHUNKS):
        if c == CHUNKS - 1:
            for s in range(min(2, near)):
                with scope(f"hand{s}"):
                    hand(s)
        with scope(f"take{c}"):
            take(c)
        with scope(f"wf{c}"):
            own_f[c].wait_recv()
        with scope(f"proj{c}"):
            project(c)
        if c < CHUNKS - 1:
            with scope(f"att{c}"):
                attend(c)
    with scope("send_near"):
        send_near()
    for s in range(2, near):
        with scope(f"hand{s}"):
            hand(s)
    with scope("attlast"):
        attend(CHUNKS - 1)

    split = near // 2
    for s in range(near):
        with scope(f"on{s}"):
            hand_on(s)
        if s == split:
            with scope("pf0"):
                project_far(0, split)
            with scope("early"):
                absorb_early(0, split)
    with scope("pf1"):
        project_far(split, near)
    with scope("take_near"):
        take_near()

    with scope("wo"):
        wo_load.wait()
    wide = cols // OUT_CHUNKS
    to_mate, to_across = [], []

    def span(c):
        return slice(c * wide, (c + 1) * wide)

    def share(which, part):
        psend[which] = dot(att[part, :], wobuf[...]).astype(BF)
        for c in range(OUT_CHUNKS):
            i = which * OUT_CHUNKS + c
            x = remote(
                psend.at[which, :, span(c)],
                precv.at[which, :, span(c)],
                pd_s.at[i],
                pd_r.at[i],
                (me, mate),
            )
            x.start()
            to_mate.append(x)

    with scope("fin0"):
        first, second = finish(split, last, diag, across)
    with scope("share0"):
        share(0, first)
    with scope("sharex"):
        part_x[...] = dot(att[second, :], wobuf[...])
    with scope("sendx"):
        for c in range(OUT_CHUNKS):
            to_mate[c].wait_recv()
            xsend[:, span(c)] = (part_x[:, span(c)] + precv[0, :, span(c)].astype(F32)).astype(BF)
            here = pl.ds(0, quarter), pl.ds(c * wide, wide)
            x = remote(xsend.at[here], xrecv.at[here], px_s.at[c], px_r.at[c], (me, across))
            x.start()
            to_across.append(x)
    with scope("fin1"):
        first, second = finish(split, last, mate, t)
    with scope("share1"):
        share(1, first)
    with scope("mine"):
        mine[...] = dot(att[second, :], wobuf[...])
        for c in range(OUT_CHUNKS):
            to_mate[OUT_CHUNKS + c].wait_recv()
        mine[...] += precv[1].astype(F32)
    with scope("out"):
        for c in range(OUT_CHUNKS):
            to_across[c].wait_recv()
            out[:, span(c)] = (mine[:, span(c)] + xrecv[:, span(c)].astype(F32)).astype(BF)

    with scope("drain"):
        for c in own_x + [own_c] + own_f + to_mate + to_across:
            c.wait_send()
        for k in range(1, n):
            pl.when(me >= k)(asks[k - 1].wait_send)
            pl.when((me < near) & (me + k < n))(sends[k].wait_send)
        for k in range(1, reach + 1):
            pl.when((me >= near) & (me + k < n))(near_sends[k - 1].wait_send)
        for s in range(near):

            @pl.when(me > s)
            def _():
                far_x[s].wait_send()
                far_c[s].wait_send()
                far_f[s].wait_send()


def local(n, tokens, w_query, w_key, w_value, w_out, chosen):
    rows, feat = tokens.shape
    depth, width = w_query.shape
    heads = width // HD
    cols = w_out.shape[1]
    blocks = n * (rows // BLK)
    slot = MOST * BLK
    near = n // 2
    reach = n - 1 - near
    used = (n - 1) * slot
    quarter = rows // 4
    vmem = pl.BlockSpec(memory_space=pltpu.VMEM)
    hbm = pl.BlockSpec(memory_space=pltpu.HBM)
    dma = pltpu.SemaphoreType.DMA
    V = pltpu.VMEM
    many = dma((n - 1,))
    some = dma((CHUNKS,))
    return pl.pallas_call(
        functools.partial(kernel, n),
        out_shape=jax.ShapeDtypeStruct((quarter, cols), BF),
        in_specs=[hbm] * 6,
        out_specs=vmem,
        scratch_shapes=[
            V(chosen.shape, jnp.int32),
            V((depth, 3 * width), BF),
            V((width, cols), BF),
            V((rows, depth), BF),
            V((near * slot, depth), BF),
            V((n - 1, slot, feat), BF),
            V((reach * slot, 2 * width), BF),
            V((n, 8, rows), F32),
            V((n - 1, 8, rows), F32),
            V((reach * slot, rows), BF),
            V((rows, 3 * width), BF),
            V((used, 2 * width), BF),
            V((rows, rows), F32),
            V((rows, used), F32),
            V((heads, rows, 1), F32),
            V((heads, rows, 1), F32),
            V((heads, rows, HD), F32),
            V((rows, width), BF),
            V((2, quarter, cols), BF),
            V((2, quarter, cols), BF),
            V((quarter, cols), F32),
            V((quarter, cols), BF),
            V((quarter, cols), BF),
            V((quarter, cols), F32),
            dma((6,)),
            some, some,
            dma, dma,
            some, some,
            many, many,
            many, many,
            many, many,
            many, many,
            many, many,
            dma((2 * OUT_CHUNKS,)), dma((2 * OUT_CHUNKS,)),
            dma((OUT_CHUNKS,)), dma((OUT_CHUNKS,)),
        ],
        compiler_params=pltpu.CompilerParams(
            collective_id=0, has_side_effects=True, vmem_limit_bytes=VMEM_MIB * 1024 * 1024
        ),
    )(tokens, w_query, w_key, w_value, w_out, chosen)


def solution(mesh):
    return jax.shard_map(
        functools.partial(local, mesh.shape["kv"]),
        mesh=mesh,
        in_specs=(
            P("kv", "tp"),
            P(None, "tp"),
            P(None, "tp"),
            P(None, "tp"),
            P("tp", None),
            P("kv", None),
        ),
        out_specs=P(("kv", "tp"), None),
        check_vma=False,
    )
```

```python
import functools

import jax
import jax.numpy as jnp
from jax import lax
from jax.experimental import pallas as pl
from jax.experimental.pallas import tpu as pltpu
from jax.sharding import PartitionSpec as P

HD = 128
BLK = 32
MOST = 2
NEG = -1e30
LOG2E = 1.4426950408889634
BF = jnp.bfloat16
F32 = jnp.float32
MESH = pl.DeviceIdType.MESH
CHUNKS = 4
OUT_CHUNKS = 4
VMEM_MIB = 60
scope = jax.named_scope


def dot(a, b):
    return jnp.dot(a, b, preferred_element_type=F32)


def dot_nt(a, b):
    return lax.dot_general(a, b, (((1,), (1,)), ((), ())), preferred_element_type=F32)


def quot(x, size):
    if size & (size - 1) == 0:
        return lax.shift_right_logical(x, jnp.full(x.shape, size.bit_length() - 1, x.dtype))
    return lax.div(x, size)


def rest(x, size):
    if size & (size - 1) == 0:
        return x & (size - 1)
    return lax.rem(x, size)


def iota(shape, dim):
    return lax.broadcasted_iota(jnp.int32, shape, dim)


def ones_where(cond):
    return cond.astype(F32).astype(BF)


def kernel(
    n, tok, wq, wk, wv, wo, chosen, out,
    rowsel, wbuf, wobuf, gat, far, pick, pickf, ask, asked, choice, qkv, kvf,
    bias, biasf, top, tot, summed, att, psend, precv, part_x, xsend, xrecv, mine,
    wsem, ox_s, ox_r, oc_s, oc_r, of_s, of_r, rq_s, rq_r, fk_s, fk_r,
    fx_s, fx_r, fc_s, fc_r, ff_s, ff_r, pd_s, pd_r, px_s, px_r,
):
    rows, feat = tok.shape
    width = wq.shape[1]
    heads = width // HD
    per = rows // BLK
    blocks = n * per
    slot = MOST * BLK
    spots = kvf.shape[0]
    cols = wo.shape[1]
    quarter = rows // 4
    piece = rows // CHUNKS
    me = lax.axis_index("kv")
    t = lax.axis_index("tp")
    mate = t + 1 - 2 * lax.rem(t, 2)
    across = lax.rem(t + 2, 4)
    diag = lax.rem(mate + 2, 4)
    last = n - 1
    near = n // 2
    reach = last - near

    def has(s):
        if s >= near:
            return me > s
        return jnp.where(me >= near, True, (s > 0) & (me >= s))

    def lanes(d):
        return pl.ds(pl.multiple_of(d * feat, feat), feat)

    def remote(src, dst, s, r, who):
        return pltpu.make_async_remote_copy(
            src_ref=src, dst_ref=dst, send_sem=s, recv_sem=r, device_id=who, device_id_type=MESH
        )

    barrier = pltpu.get_barrier_semaphore()
    for d in (mate, across, diag):
        pl.semaphore_signal(barrier, inc=1, device_id=(me, d), device_id_type=MESH)
    for k in range(1, n):
        pl.semaphore_signal(
            barrier, inc=1, device_id=(lax.rem(me + k, n), t), device_id_type=MESH
        )

    list_load = pltpu.make_async_copy(chosen, rowsel, wsem.at[5])
    list_load.start()
    tok_load = pltpu.make_async_copy(tok, gat.at[:, lanes(t)], wsem.at[0])
    tok_load.start()
    loads = []
    for j, w in enumerate((wq, wk, wv)):
        c = pltpu.make_async_copy(w, wbuf.at[:, pl.ds(j * width, width)], wsem.at[1 + j])
        c.start()
        loads.append(c)
    wo_load = pltpu.make_async_copy(wo, wobuf, wsem.at[4])
    wo_load.start()

    with scope("ask"):
        lane = iota((per, blocks), 1)
        seen = jnp.zeros((per, blocks), jnp.int32)
        list_load.wait()
        picks = rowsel[...]
        for j in range(picks.shape[1]):
            seen = jnp.maximum(seen, (picks[:, j : j + 1] == lane).astype(jnp.int32))
        wanted = jnp.max(seen, axis=0, keepdims=True)
        lane1 = iota((1, blocks), 1)
        inside = (lane1 >= me * per) & (lane1 < me * per + per)
        wanted = jnp.where(inside, 0, wanted).astype(F32)
        ia, ib = iota((blocks, blocks), 0), iota((blocks, blocks), 1)
        tri = ones_where((quot(ia, per) == quot(ib, per)) & (ia <= ib))
        rank = dot(jnp.broadcast_to(wanted, (8, blocks)).astype(BF), tri)[0:1, :] * wanted
        pad = max(n, 8)
        owner = quot(iota((pad, blocks), 1), per) == iota((pad, blocks), 0)
        ranks = jnp.where(owner, jnp.broadcast_to(rank, (pad, blocks)), 0.0).astype(BF)
        within = ones_where(
            rest(iota((blocks, rows), 0), per) == quot(iota((blocks, rows), 1), BLK)
        )
        places = dot(ranks, within)
        for s in range(n):
            ask[s] = places[s : s + 1, :]

    tok_load.wait()
    with scope("barrier"):
        pl.semaphore_wait(barrier, n + 2)

    own_x, own_f = [], []
    for c in range(CHUNKS):
        part = pl.ds(c * piece, piece)
        src = gat.at[part, lanes(t)]
        own_x.append(remote(src, src, ox_s.at[c], ox_r.at[c], (me, across)))
        own_x[-1].start()
    whole = gat.at[:, lanes(t)]
    own_c = remote(whole, whole, oc_s, oc_r, (me, mate))
    own_c.start()

    asks = []
    for k in range(1, n):
        low = lax.max(me - k, 0)
        c = remote(ask.at[low], asked.at[k - 1], rq_s.at[k - 1], rq_r.at[k - 1], (low, t))
        pl.when(me >= k)(c.start)
        asks.append(c)

    with scope("bias"):
        seen_b = seen.astype(F32).astype(BF)
        spread = ones_where(iota((blocks, rows), 0) == me * per + quot(iota((blocks, rows), 1), BLK))
        col = iota((spots, blocks), 0)
        blk = iota((spots, blocks), 1)
        place = quot(col, slot)
        source = me - place
        source = jnp.where(source < 0, source + near, source)
        source = jnp.where(source >= near, source - near, source)
        source = jnp.where(place < near, source, place)
        hit = ones_where(
            (source == quot(blk, per))
            & (
                jnp.broadcast_to(rank, (spots, blocks))
                == (quot(rest(col, slot), BLK) + 1).astype(F32)
            )
        )
        far_seen = dot_nt(seen_b, hit)
        grow = ones_where(quot(iota((rows, per), 0), BLK) == iota((rows, per), 1))
        own_seen = dot(grow, dot(seen_b, spread).astype(BF))
        causal = iota((rows, rows), 1) <= iota((rows, rows), 0)
        bias[...] = jnp.where((own_seen > 0.5) & causal, 0.0, NEG)
        biasf[...] = jnp.where(dot(grow, far_seen.astype(BF)) > 0.5, 0.0, NEG)
        for s in range(last):
            part = pl.ds(s * slot, slot)

            @pl.when(jnp.logical_not(has(s)))
            def _():
                if s < near:
                    far[part, :] = jnp.zeros((slot, far.shape[1]), BF)
                kvf[part, :] = jnp.zeros((slot, kvf.shape[1]), BF)

    with scope("picks"):
        srow, scol = iota((slot, rows), 0), iota((slot, rows), 1)
        same = rest(srow, BLK) == rest(scol, BLK)
        want_rank = (quot(srow, BLK) + 1).astype(F32)
        sends = {}

        def select(k):
            sel = same & (asked[k - 1] == want_rank)
            return ones_where(sel)

        for k in range(1, n):
            sends[k] = remote(
                pick.at[k - 1],
                far.at[pl.ds(k % near * slot, slot), lanes(t)],
                fk_s.at[k - 1],
                fk_r.at[k % near],
                (lax.rem(me + k, n), t),
            )

        def token_send(k, when):
            @pl.when((me < near) & when)
            def _():
                asks[k - 1].wait_recv()
                pick[k - 1] = dot(select(k), gat[:, lanes(t)]).astype(BF)
                sends[k].start()

        for j in range(near):
            token_send(near + j, me + near + j < n)
            if j:
                token_send(j, me + j >= near)
        for j in range(1, near):
            token_send(j, me + j < near)

        @pl.when(me >= near)
        def _():
            for k in range(1, reach + 1):

                @pl.when(me + k < n)
                def _():
                    asks[k - 1].wait_recv()
                    choice[pl.ds((k - 1) * slot, slot), :] = select(k)

                @pl.when(me + k >= n)
                def _():
                    choice[pl.ds((k - 1) * slot, slot), :] = jnp.zeros((slot, rows), BF)

    scale = HD ** (-0.5) * LOG2E
    cut = [slice(h * HD, (h + 1) * HD) for h in range(heads)]

    def head(j, h):
        return slice(j * width + h * HD, j * width + (h + 1) * HD)

    def project(c, lo, hi):
        rr = slice(c * piece, (c + 1) * piece)
        val = dot(gat[rr, :], wbuf[:, lo * width : hi * width])
        if lo == 0:
            qkv[rr, :width] = (val[:, :width] * scale).astype(BF)
            val = val[:, width:]
        if hi == 3:
            qkv[rr, width:] = val.astype(BF)

    def attend(c):
        rr = slice(c * piece, (c + 1) * piece)
        upto = (c + 1) * piece
        shade = bias[rr, :upto]
        ss = [dot_nt(qkv[rr, head(0, h)], qkv[:upto, head(1, h)]) + shade for h in range(heads)]
        ms = [jnp.max(x, axis=1, keepdims=True) for x in ss]
        ps = [jnp.exp2(x - m) for x, m in zip(ss, ms)]
        vals = [dot(p.astype(BF), qkv[:upto, head(2, h)]) for h, p in enumerate(ps)]
        for h in range(heads):
            top[h, rr, :] = ms[h]
            tot[h, rr, :] = jnp.sum(ps[h], axis=1, keepdims=True)
            summed[h, rr, :] = vals[h]

    near_sends = []

    def send_near():
        for k in range(1, reach + 1):
            part = pl.ds((k - 1) * slot, slot)
            near_sends.append(
                remote(
                    pickf.at[part],
                    kvf.at[pl.ds(pl.multiple_of(me * slot, slot), slot)],
                    fk_s.at[k - 1],
                    fk_r.at[me],
                    (lax.rem(me + k, n), t),
                )
            )

        @pl.when((me >= near) & (me < last))
        def _():
            pickf[...] = dot(choice[...], qkv[:, width:]).astype(BF)
            for k in range(reach, 0, -1):
                pl.when(me + k < n)(near_sends[k - 1].start)

    def take_near():
        for s in range(near, last):

            @pl.when(me > s)
            def _():
                here = kvf.at[slot_of(s)]
                remote(here, here, fk_s.at[0], fk_r.at[s], (me, t)).wait_recv()

    far_x, far_c, far_f = [], [], []

    def slot_of(s):
        return pl.ds(s * slot, slot)

    def hand(s):
        here = far.at[slot_of(s), lanes(t)]
        far_x.append(remote(here, here, fx_s.at[s], fx_r.at[s], (me, across)))
        far_c.append(remote(here, here, fc_s.at[s], fc_r.at[s], (me, mate)))

        @pl.when(has(s))
        def _():
            remote(pick.at[0], here, fk_s.at[0], fk_r.at[s], (me, t)).wait_recv()
            far_x[s].start()
            far_c[s].start()

    def hand_on(s):
        theirs = far.at[slot_of(s), lanes(across)]
        far_f.append(remote(theirs, theirs, ff_s.at[s], ff_r.at[s], (me, mate)))

        @pl.when(has(s))
        def _():
            far_x[s].wait_recv()
            far_f[s].start()

    def any_of(lo, hi):
        if lo >= near:
            return me > lo
        return (me >= near) | (me >= max(lo, 1))

    def project_far(lo, hi):
        @pl.when(any_of(lo, hi))
        def _():
            for s in range(lo, hi):

                @pl.when(has(s))
                def _():
                    far_c[s].wait_recv()
                    far_f[s].wait_recv()

            part = slice(lo * slot, hi * slot)
            kvf[part, :] = dot(far[part, :], wbuf[:, width:]).astype(BF)

    def absorb(part, lo, hi):
        keys = slice(lo * slot, hi * slot)
        shade = biasf[part, keys]
        ss = [dot_nt(qkv[part, head(0, h)], kvf[keys, cut[h]]) + shade for h in range(heads)]
        old = [top[h, part, :] for h in range(heads)]
        ms = [jnp.maximum(m, jnp.max(x, axis=1, keepdims=True)) for m, x in zip(old, ss)]
        ps = [jnp.exp2(x - m) for x, m in zip(ss, ms)]
        keep = [jnp.exp2(m0 - m) for m0, m in zip(old, ms)]
        vals = [dot(p.astype(BF), kvf[keys, width + h * HD : width + (h + 1) * HD]) for h, p in enumerate(ps)]
        totals = [tot[h, part, :] * keep[h] + jnp.sum(ps[h], axis=1, keepdims=True) for h in range(heads)]
        sums = [summed[h, part, :] * keep[h] + vals[h] for h in range(heads)]
        return ms, totals, sums

    def absorb_early(lo, hi):
        @pl.when(any_of(lo, hi))
        def _():
            for r in range(2):
                part = slice(2 * r * quarter, 2 * (r + 1) * quarter)
                ms, totals, sums = absorb(part, lo, hi)
                for h in range(heads):
                    top[h, part, :] = ms[h]
                    tot[h, part, :] = totals[h]
                    summed[h, part, :] = sums[h]

    def finish(lo, hi, *whos):
        parts = [pl.ds(pl.multiple_of(who * quarter, quarter), quarter) for who in whos]

        @pl.when(any_of(lo, hi))
        def _():
            for part in parts:
                _, totals, sums = absorb(part, lo, hi)
                for h in range(heads):
                    att[part, cut[h]] = (sums[h] / totals[h]).astype(BF)

        @pl.when(jnp.logical_not(any_of(lo, hi)))
        def _():
            for part in parts:
                for h in range(heads):
                    att[part, cut[h]] = (summed[h, part, :] / tot[h, part, :]).astype(BF)

        return parts

    for c in loads:
        c.wait()

    with scope("own_c"):
        own_c.wait_recv()

    def take(c):
        own_x[c].wait_recv()
        theirs = gat.at[pl.ds(c * piece, piece), lanes(across)]
        own_f.append(remote(theirs, theirs, of_s.at[c], of_r.at[c], (me, mate)))
        own_f[c].start()

    def step(name, act, *args):
        with scope(name):
            act(*args)

    final = CHUNKS - 1
    step("take0", take, 0)
    for c in range(CHUNKS):
        if c == final - 2:
            step("hand0", hand, 0)
        if c and c < final:
            step(f"take{c}", take, c)
            step(f"att{c - 1}", attend, c - 1)
        if c == final - 1:
            step("hand1", hand, 1)
            step(f"take{final}", take, final)
        step(f"wf{c}", own_f[c].wait_recv)
        if c < final:
            step(f"proj{c}", project, c, 0, 3)
    step("hand2", hand, 2)
    step(f"proj{final}", project, final, 1, 3)
    step("send_near", send_near)
    for s in range(3, near):
        step(f"hand{s}", hand, s)
    step("attm", attend, final - 1)
    step(f"projq", project, final, 0, 1)
    step("attlast", attend, final)

    split = near // 2
    for s in range(near):
        step(f"on{s}", hand_on, s)
        if s == split:
            step("pf0", project_far, 0, split)
    step("early", absorb_early, 0, split)
    with scope("pf1"):
        project_far(split, near)
    with scope("take_near"):
        take_near()

    with scope("wo"):
        wo_load.wait()
    wide = cols // OUT_CHUNKS
    to_mate, to_across = [], []

    def span(c):
        return slice(c * wide, (c + 1) * wide)

    def share(which, part):
        psend[which] = dot(att[part, :], wobuf[...]).astype(BF)
        for c in range(OUT_CHUNKS):
            i = which * OUT_CHUNKS + c
            x = remote(
                psend.at[which, :, span(c)],
                precv.at[which, :, span(c)],
                pd_s.at[i],
                pd_r.at[i],
                (me, mate),
            )
            x.start()
            to_mate.append(x)

    with scope("fin0"):
        first, second = finish(split, last, diag, across)
    with scope("share0"):
        share(0, first)
    with scope("sharex"):
        part_x[...] = dot(att[second, :], wobuf[...])
    with scope("sendx"):
        for c in range(OUT_CHUNKS):
            to_mate[c].wait_recv()
            xsend[:, span(c)] = (part_x[:, span(c)] + precv[0, :, span(c)].astype(F32)).astype(BF)
            here = pl.ds(0, quarter), pl.ds(c * wide, wide)
            x = remote(xsend.at[here], xrecv.at[here], px_s.at[c], px_r.at[c], (me, across))
            x.start()
            to_across.append(x)
    with scope("fin1"):
        first, second = finish(split, last, mate, t)
    with scope("share1"):
        share(1, first)
    with scope("mine"):
        mine[...] = dot(att[second, :], wobuf[...])
        for c in range(OUT_CHUNKS):
            to_mate[OUT_CHUNKS + c].wait_recv()
        mine[...] += precv[1].astype(F32)
    with scope("out"):
        for c in range(OUT_CHUNKS):
            to_across[c].wait_recv()
            out[:, span(c)] = (mine[:, span(c)] + xrecv[:, span(c)].astype(F32)).astype(BF)

    with scope("drain"):
        for c in own_x + [own_c] + own_f + to_mate + to_across:
            c.wait_send()
        for k in range(1, n):
            pl.when(me >= k)(asks[k - 1].wait_send)
            pl.when((me < near) & (me + k < n))(sends[k].wait_send)
        for k in range(1, reach + 1):
            pl.when((me >= near) & (me + k < n))(near_sends[k - 1].wait_send)
        for s in range(near):

            @pl.when(has(s))
            def _():
                far_x[s].wait_send()
                far_c[s].wait_send()
                far_f[s].wait_send()


def local(n, tokens, w_query, w_key, w_value, w_out, chosen):
    rows, feat = tokens.shape
    depth, width = w_query.shape
    heads = width // HD
    cols = w_out.shape[1]
    blocks = n * (rows // BLK)
    slot = MOST * BLK
    near = n // 2
    reach = n - 1 - near
    used = (n - 1) * slot
    quarter = rows // 4
    vmem = pl.BlockSpec(memory_space=pltpu.VMEM)
    hbm = pl.BlockSpec(memory_space=pltpu.HBM)
    dma = pltpu.SemaphoreType.DMA
    V = pltpu.VMEM
    many = dma((n - 1,))
    some = dma((CHUNKS,))
    return pl.pallas_call(
        functools.partial(kernel, n),
        out_shape=jax.ShapeDtypeStruct((quarter, cols), BF),
        in_specs=[hbm] * 6,
        out_specs=vmem,
        scratch_shapes=[
            V(chosen.shape, jnp.int32),
            V((depth, 3 * width), BF),
            V((width, cols), BF),
            V((rows, depth), BF),
            V((near * slot, depth), BF),
            V((n - 1, slot, feat), BF),
            V((reach * slot, 2 * width), BF),
            V((n, 1, rows), F32),
            V((n - 1, 1, rows), F32),
            V((reach * slot, rows), BF),
            V((rows, 3 * width), BF),
            V((used, 2 * width), BF),
            V((rows, rows), F32),
            V((rows, used), F32),
            V((heads, rows, 1), F32),
            V((heads, rows, 1), F32),
            V((heads, rows, HD), F32),
            V((rows, width), BF),
            V((2, quarter, cols), BF),
            V((2, quarter, cols), BF),
            V((quarter, cols), F32),
            V((quarter, cols), BF),
            V((quarter, cols), BF),
            V((quarter, cols), F32),
            dma((6,)),
            some, some,
            dma, dma,
            some, some,
            many, many,
            many, many,
            many, many,
            many, many,
            many, many,
            dma((2 * OUT_CHUNKS,)), dma((2 * OUT_CHUNKS,)),
            dma((OUT_CHUNKS,)), dma((OUT_CHUNKS,)),
        ],
        compiler_params=pltpu.CompilerParams(
            collective_id=0, has_side_effects=True, vmem_limit_bytes=min(63, 30 + n * 3 // 2) * 1024 * 1024
        ),
    )(*(pltpu.with_memory_space_constraint(x, pltpu.HBM) for x in (tokens, w_query, w_key, w_value, w_out, chosen)))


def solution(mesh):
    return jax.shard_map(
        functools.partial(local, mesh.shape["kv"]),
        mesh=mesh,
        in_specs=(
            P("kv", "tp"),
            P(None, "tp"),
            P(None, "tp"),
            P(None, "tp"),
            P("tp", None),
            P("kv", None),
        ),
        out_specs=P(("kv", "tp"), None),
        check_vma=False,
    )
```
